32 devices in a mesh: grp: 2 (over y), sp: 4 (over z), tp: 4 (over x, core).
Axes of the slice: x: 2, y: 2, z: 4, core: 2. Of those that a mesh axis runs over, the one named last changes fastest.
Arguments:
- tokens: bfloat16 [3072, 4096], P(('grp', 'sp'), 'tp'), parts along dimension 0, may hold values from -6 to 6
- proj_b: bfloat16 [2, 4096, 2048], P(None, 'sp', 'tp'), may hold values from -0.09375 to 0.09375
- proj_c: bfloat16 [2, 4096, 2048], P(None, 'sp', 'tp'), may hold values from -0.09375 to 0.09375
- proj_x: bfloat16 [2, 4096, 2048], P(None, 'sp', 'tp'), may hold values from -0.09375 to 0.09375
- proj_out: bfloat16 [2, 2048, 4096], P(None, 'sp', 'tp'), may hold values from -1 to 1
- conv_taps: float32 [2, 3, 2048], P(None, None, 'tp'), may hold values from -3 to 3
- ln_gain: float32 [2, 4096], P(None, 'tp'), may hold values from 0.1 to 1.9
- ln_bias: float32 [2, 4096], P(None, 'tp'), may hold values from -2 to 2
Outputs:
- result: bfloat16 [3072, 4096], P(('grp', 'sp'), 'tp'), parts along dimension 0
The draws below stay inside these ranges and needn't reach their ends.
There are 2 independent parts, one for each index of `grp`. The reference program is written for one: setup_inputs(seed, part) draws one part's arguments, and reference() takes and returns one part's arrays. A program takes and returns all parts, laid end to end along the dimension named above; an argument that names none is the same for every part. Nothing has to cross between parts.
All inputs are finite; a program needn't handle non-finite values.
Results may differ from the reference program's by a relative error of at most 0.012.
Values may be sent and summed in bfloat16 or wider, within the bound.
A program may use at most 128 MiB of HBM per device.

```python
import jax
import jax.numpy as jnp
from jax import lax

D = 4096
CW = 2048
KW = 3
LAYERS = 2
TOKENS = 1536


def draw_proj_out(key, part):
    first_key = jax.random.fold_in(key, 11)
    second_key = jax.random.fold_in(key, 12)
    column_pos = jnp.arange(D, dtype=jnp.float32) / D
    jitter = jax.random.uniform(second_key, (LAYERS, 1, D), jnp.float32, -0.35, 0.35)
    entries = jax.random.normal(first_key, (LAYERS, CW, D), jnp.float32)
    ramp = jnp.exp(jnp.log(6.0) * column_pos)
    scaled = entries * CW ** (-0.5) * ramp * jnp.exp(jitter) / 2.5
    return jnp.clip(scaled, -1.0, 1.0).astype(jnp.bfloat16)


def block_levels(own_key, extent, shards, low, high):
    def one(dim, blocks):
        heights = jax.random.uniform(jax.random.fold_in(jax.random.fold_in(own_key, 6), dim), (blocks,), jnp.float32, low / len(shards), high / len(shards))
        return jnp.repeat(jnp.exp(heights), extent[dim] // blocks).reshape((-1,) + (1,) * (len(extent) - dim - 1))

    loudness = one(*shards[0])
    for cut in shards[1:]:
        loudness = loudness * one(*cut)
    return loudness


def centred(rng, shape, deviation, reach, split=(), held_as=jnp.bfloat16):
    factor_of = block_levels(rng, shape, split, -0.22, 0.18) if split else 1.0
    values = jax.random.normal(rng, shape, jnp.float32) * deviation * factor_of
    return jnp.minimum(jnp.maximum(values, -reach), reach).astype(held_as)


def setup_inputs(seed: int = 0, part: int = 0) -> dict:
    streams_of = jax.random.split(jax.random.key(seed), 9)
    part_keys = jax.random.split(jax.random.fold_in(streams_of[8], part), 9)
    tokens = centred(part_keys[0], (TOKENS, D), 1.0, 6.0, ((0, 4), (1, 4)))
    proj_b = centred(streams_of[1], (LAYERS, D, CW), D ** -0.5, 0.09375, ((1, 4), (2, 4)))
    proj_c = centred(streams_of[2], (LAYERS, D, CW), D ** -0.5, 0.09375, ((1, 4), (2, 4)))
    proj_x = centred(streams_of[3], (LAYERS, D, CW), D ** -0.5, 0.09375, ((1, 4), (2, 4)))
    proj_out = draw_proj_out(jax.random.fold_in(streams_of[8], 71), part)
    conv_taps = centred(streams_of[5], (LAYERS, KW, CW), 0.6, 3.0, ((2, 4),), jnp.float32)
    ln_gain = jnp.clip(1.0 + 0.18 * jax.random.normal(streams_of[6], (LAYERS, D), jnp.float32), 0.1, 1.9)
    ln_bias = centred(streams_of[7], (LAYERS, D), 0.3, 2.0, ((1, 4),), jnp.float32)
    return {"tokens": tokens, "proj_b": proj_b, "proj_c": proj_c, "proj_x": proj_x, "proj_out": proj_out, "conv_taps": conv_taps, "ln_gain": ln_gain, "ln_bias": ln_bias}


norm_eps = 1e-05

def reference(tokens, proj_b, proj_c, proj_x, proj_out, conv_taps, ln_gain, ln_bias):
    residual_scale = (2.0 * LAYERS) ** 0.25
    hidden = tokens
    for layer_index in range(LAYERS):
        out_gate = lax.optimization_barrier(jnp.dot(hidden, proj_b[layer_index], preferred_element_type=jnp.float32).astype(jnp.bfloat16))
        in_gate = lax.optimization_barrier(jnp.dot(hidden, proj_c[layer_index], preferred_element_type=jnp.float32).astype(jnp.bfloat16))
        values = lax.optimization_barrier(jnp.dot(hidden, proj_x[layer_index], preferred_element_type=jnp.float32).astype(jnp.bfloat16))
        gated_in = in_gate.astype(jnp.float32) * values.astype(jnp.float32)
        count_rows = gated_in.shape[0]
        padded = jnp.concatenate([jnp.zeros((KW - 1, gated_in.shape[1]), jnp.float32), gated_in], 0)
        conv_out = jnp.zeros_like(gated_in)
        for tap_index in range(KW):
            conv_out = conv_out + conv_taps[layer_index, tap_index] * padded[tap_index:tap_index + count_rows]
        branch = (out_gate.astype(jnp.float32) * conv_out).astype(jnp.bfloat16)
        mixed = lax.optimization_barrier(jnp.dot(branch, proj_out[layer_index], preferred_element_type=jnp.float32).astype(jnp.bfloat16))
        summed = residual_scale * hidden.astype(jnp.float32) + mixed.astype(jnp.float32)
        mean = lax.optimization_barrier(jnp.mean(summed, axis=1, keepdims=True))
        centered = summed - mean
        variance = lax.optimization_barrier(jnp.mean(centered * centered, axis=1, keepdims=True))
        hidden = (centered * lax.rsqrt(variance + norm_eps) * ln_gain[layer_index] + ln_bias[layer_index]).astype(jnp.bfloat16)
    return hidden
```

```python
import jax
import jax.numpy as jnp
from jax import lax
from jax.sharding import PartitionSpec as P

LAYERS = 2


norm_eps = 1e-05


def from_behind(block, axis, distance):
    devices = range(lax.axis_size(axis))
    route = [(i - distance, i) for i in devices if i - distance in devices]
    return lax.ppermute(block, axis, route)


def local(tokens, proj_b, proj_c, proj_x, proj_out, conv_taps, ln_gain, ln_bias):
    residual_scale = (2.0 * LAYERS) ** 0.25
    parts = lax.axis_size("grp")
    me = lax.axis_index("grp")
    rows = tokens.shape[0]
    wide = proj_b.shape[2] // parts
    out_wide = proj_out.shape[2] // parts

    def mine(array, width):
        return lax.dynamic_slice_in_dim(array, me * width, width, array.ndim - 1)

    weights = []
    for layer_index in range(LAYERS):
        ins = jnp.concatenate(
            [mine(w[layer_index], wide) for w in (proj_b, proj_c, proj_x)], axis=1
        )
        weights.append(
            (
                lax.all_gather(ins, "sp", axis=0, tiled=True),
                lax.all_gather(mine(proj_out[layer_index], out_wide), "sp", axis=0, tiled=True),
            )
        )
    taps, gain, bias = mine(conv_taps, wide), mine(ln_gain, out_wide), mine(ln_bias, out_wide)
    swapped = lax.all_to_all(
        tokens.reshape(rows, parts, out_wide), "grp", split_axis=1, concat_axis=0, tiled=False
    )
    hidden = swapped.reshape(parts * rows, out_wide)
    reach = taps.shape[1] - 1
    for layer_index in range(LAYERS):
        whole_in, whole_out = weights[layer_index]
        gathered = lax.all_gather(hidden, ("tp", "grp"), axis=1, tiled=True)
        acc = jnp.dot(gathered, whole_in, preferred_element_type=jnp.float32)
        acc = lax.optimization_barrier(acc.astype(jnp.bfloat16)).astype(jnp.float32)
        out_gate, in_gate, values = (acc[:, i * wide : (i + 1) * wide] for i in range(3))
        gated_in = (in_gate * values).reshape(parts, rows, wide)
        fringe = from_behind(gated_in[:, rows - reach :], "sp", 1)
        padded = jnp.concatenate([fringe, gated_in], 1)
        conv_out = jnp.zeros_like(gated_in)
        for tap_index in range(reach + 1):
            conv_out = (
                conv_out + taps[layer_index, tap_index] * padded[:, tap_index : tap_index + rows]
            )
        branch = (out_gate * conv_out.reshape(parts * rows, wide)).astype(jnp.bfloat16)
        all_branch = lax.all_gather(branch, ("tp", "grp"), axis=1, tiled=True)
        acc_out = jnp.dot(all_branch, whole_out, preferred_element_type=jnp.float32)
        mixed = lax.optimization_barrier(acc_out.astype(jnp.bfloat16))
        summed = residual_scale * hidden.astype(jnp.float32) + mixed.astype(jnp.float32)
        width_all = summed.shape[1] * lax.axis_size(("tp", "grp"))
        mean = (lax.psum(jnp.sum(summed, axis=1), ("tp", "grp")) / width_all)[:, None]
        centered = summed - mean
        variance = (lax.psum(jnp.sum(centered * centered, axis=1), ("tp", "grp")) / width_all)[
            :, None
        ]
        hidden = (
            centered * lax.rsqrt(variance + norm_eps) * gain[layer_index] + bias[layer_index]
        ).astype(jnp.bfloat16)
    back = lax.all_to_all(
        hidden.reshape(parts, rows, out_wide), "grp", split_axis=0, concat_axis=1, tiled=False
    )
    return back.reshape(rows, parts * out_wide)


def solution(mesh):
    return jax.shard_map(
        local,
        mesh=mesh,
        in_specs=(
            P(("grp", "sp"), "tp"),
            P(None, "sp", "tp"),
            P(None, "sp", "tp"),
            P(None, "sp", "tp"),
            P(None, "sp", "tp"),
            P(None, None, "tp"),
            P(None, "tp"),
            P(None, "tp"),
        ),
        out_specs=P(("grp", "sp"), "tp"),
        check_vma=False,
    )
```

```python
import jax
import jax.numpy as jnp
from jax import lax
from jax.sharding import PartitionSpec as P

LAYERS = 2


norm_eps = 1e-05


def from_behind(block, axis, distance):
    devices = range(lax.axis_size(axis))
    route = [(i - distance, i) for i in devices if i - distance in devices]
    return lax.ppermute(block, axis, route)


def along_line(block, axis, earlier):
    size = lax.axis_size(axis)
    blocks, latest = [(0, block)], []
    for side, step in enumerate((1, -1)):
        moving = block
        if earlier:
            moving, _ = lax.optimization_barrier((moving, earlier[side]))
        hops = []
        for hop in range(1, size):
            start = range(hop - 1, size - 1) if step == 1 else range(1, size - hop + 1)
            moving = lax.ppermute(moving, axis, [(i, i + step) for i in start])
            hops.append((-step * hop, moving))
        latest.append(hops[max(len(hops) - 2, 0)][1])
        blocks += hops
    return sorted(blocks, key=lambda b: abs(b[0])), latest


def dot_by_blocks(left, blocks, here, size):
    total = None
    for offset, block in blocks:
        depth = block.shape[0]
        owner = jnp.clip(here + offset, 0, size - 1)
        columns = lax.dynamic_slice_in_dim(left, owner * depth, depth, 1)
        term = jnp.dot(columns, block, preferred_element_type=jnp.float32)
        total = term if total is None else total + term
    return total


def local(tokens, proj_b, proj_c, proj_x, proj_out, conv_taps, ln_gain, ln_bias):
    residual_scale = (2.0 * LAYERS) ** 0.25
    parts = lax.axis_size("grp")
    me = lax.axis_index("grp")
    rows = tokens.shape[0]
    wide = proj_b.shape[2] // parts
    out_wide = proj_out.shape[2] // parts

    def mine(array, width):
        return lax.dynamic_slice_in_dim(array, me * width, width, array.ndim - 1)

    slabs, here = lax.axis_size("sp"), lax.axis_index("sp")
    weights = []
    earlier = None
    for layer_index in range(LAYERS):
        ins = jnp.concatenate(
            [mine(w[layer_index], wide) for w in (proj_b, proj_c, proj_x)], axis=1
        )
        ins, earlier = along_line(ins, "sp", earlier)
        outs, earlier = along_line(mine(proj_out[layer_index], out_wide), "sp", earlier)
        weights.append((ins, outs))
    taps, gain, bias = mine(conv_taps, wide), mine(ln_gain, out_wide), mine(ln_bias, out_wide)
    swapped = lax.all_to_all(
        tokens.reshape(rows, parts, out_wide), "grp", split_axis=1, concat_axis=0, tiled=False
    )
    hidden = swapped.reshape(parts * rows, out_wide)
    reach = taps.shape[1] - 1
    for layer_index in range(LAYERS):
        whole_in, whole_out = weights[layer_index]
        gathered = lax.all_gather(hidden, ("tp", "grp"), axis=1, tiled=True)
        acc = dot_by_blocks(gathered, whole_in, here, slabs)
        acc = lax.optimization_barrier(acc.astype(jnp.bfloat16)).astype(jnp.float32)
        out_gate, in_gate, values = (acc[:, i * wide : (i + 1) * wide] for i in range(3))
        gated_in = (in_gate * values).reshape(parts, rows, wide)
        fringe = from_behind(gated_in[:, rows - reach :], "sp", 1)
        padded = jnp.concatenate([fringe, gated_in], 1)
        conv_out = jnp.zeros_like(gated_in)
        for tap_index in range(reach + 1):
            conv_out = (
                conv_out + taps[layer_index, tap_index] * padded[:, tap_index : tap_index + rows]
            )
        branch = (out_gate * conv_out.reshape(parts * rows, wide)).astype(jnp.bfloat16)
        all_branch = lax.all_gather(branch, ("tp", "grp"), axis=1, tiled=True)
        acc_out = dot_by_blocks(all_branch, whole_out, here, slabs)
        mixed = lax.optimization_barrier(acc_out.astype(jnp.bfloat16))
        summed = residual_scale * hidden.astype(jnp.float32) + mixed.astype(jnp.float32)
        own_mean = jnp.mean(summed, axis=1)
        own_spread = jnp.mean(jnp.square(summed - own_mean[:, None]), axis=1)
        stats = lax.all_gather(jnp.stack([own_mean, own_spread]), ("tp", "grp"), axis=0)
        mean = jnp.mean(stats[:, 0], axis=0)
        variance = jnp.mean(stats[:, 1] + jnp.square(stats[:, 0] - mean), axis=0)[:, None]
        centered = summed - mean[:, None]
        hidden = (
            centered * lax.rsqrt(variance + norm_eps) * gain[layer_index] + bias[layer_index]
        ).astype(jnp.bfloat16)
    back = lax.all_to_all(
        hidden.reshape(parts, rows, out_wide), "grp", split_axis=0, concat_axis=1, tiled=False
    )
    return back.reshape(rows, parts * out_wide)


def solution(mesh):
    return jax.shard_map(
        local,
        mesh=mesh,
        in_specs=(
            P(("grp", "sp"), "tp"),
            P(None, "sp", "tp"),
            P(None, "sp", "tp"),
            P(None, "sp", "tp"),
            P(None, "sp", "tp"),
            P(None, None, "tp"),
            P(None, "tp"),
            P(None, "tp"),
        ),
        out_specs=P(("grp", "sp"), "tp"),
        check_vma=False,
    )
```
